32 devices in a mesh: fs: 8 (over z, x), tp: 4 (over y, core).
Axes of the slice: x: 2, y: 2, z: 4, core: 2. Of those that a mesh axis runs over, the one named last changes fastest.
Arguments:
- q_latent: bfloat16 [6144, 512], P('fs'), may hold values from -6 to 6
- q_grad: bfloat16 [6144, 3072], P('fs', 'tp'), may hold values from -6 to 6
- uq_master: float32 [512, 3072], P('fs', 'tp'), may hold values from -6 to 6
- uq_basis: bfloat16 [512, 256], P('fs'), may hold values from -4 to 4
- uq_first: float32 [256, 3072], P('fs', 'tp'), may hold values from -3 to 3
- uq_second: float32 [256, 3072], P('fs', 'tp'), may hold values from 0.1 to 1
- kv_latent: bfloat16 [6144, 512], P('fs'), may hold values from -6 to 6
- k_grad: bfloat16 [6144, 2048], P('fs', 'tp'), may hold values from -6 to 6
- uk_master: float32 [512, 2048], P('fs', 'tp'), may hold values from -6 to 6
- uk_basis: bfloat16 [512, 256], P('fs'), may hold values from -4 to 4
- uk_first: float32 [256, 2048], P('fs', 'tp'), may hold values from -3 to 3
- uk_second: float32 [256, 2048], P('fs', 'tp'), may hold values from 0.1 to 1
Outputs:
- uq_first_new: float32 [256, 3072], P('fs', 'tp')
- uq_second_new: float32 [256, 3072], P('fs', 'tp')
- uq_step: float32 [512, 3072], P('fs', 'tp')
- uq_copy: bfloat16 [512, 3072], P(None, 'tp')
- uk_first_new: float32 [256, 2048], P('fs', 'tp')
- uk_second_new: float32 [256, 2048], P('fs', 'tp')
- uk_step: float32 [512, 2048], P('fs', 'tp')
- uk_copy: bfloat16 [512, 2048], P(None, 'tp')
The draws below stay inside these ranges and needn't reach their ends.
All inputs are finite; a program needn't handle non-finite values.
Results may differ from the reference program's by a relative error of at most 0.0071.
Values may be sent and summed in bfloat16 or wider, within the bound.
A program may use at most 64 MiB of HBM per device.

```python
import math
import jax
import jax.numpy as jnp
from jax import lax

LATENT = 512
RANK = 256
TOKENS = 6144
QCOLS = 3072
KCOLS = 2048


def basis_draw(key):
    entries = jnp.clip(jax.random.normal(key, (LATENT, RANK), jnp.float32), -4.0, 4.0)
    column_scale = 10.0 ** (jnp.arange(RANK, dtype=jnp.float32) / (RANK - 1))
    return (entries * column_scale[None, :] / jnp.sqrt(LATENT * 1.0)).astype(jnp.bfloat16)


def draw_uq_basis(key, part):
    return basis_draw(jax.random.fold_in(key, 11))


def draw_uk_basis(key, part):
    return basis_draw(jax.random.fold_in(key, 12))


def strengthened(drawn, own_key, source, target, shards_of, factor):
    def block_of(axis_at):
        return (jnp.arange(drawn.shape[axis_at]) // (drawn.shape[axis_at] // shards_of)).reshape((-1,) + (1,) * (drawn.ndim - 1 - axis_at))

    near = jax.random.permutation(own_key, shards_of)[block_of(target)]
    far = (block_of(target) + shards_of // 2) % shards_of
    return jnp.where((block_of(source) == near) | (block_of(source) == far), factor * drawn, drawn)


def steps_of(own_key, shape, shards, least, largest):
    level = 1.0
    for axis_at, parts in shards:
        draws = jax.random.uniform(jax.random.fold_in(jax.random.fold_in(own_key, 6), axis_at), (parts,), jnp.float32, least / len(shards), largest / len(shards))
        level = level * jnp.repeat(jnp.exp(draws), shape[axis_at] // parts).reshape((-1,) + (1,) * (len(shape) - 1 - axis_at))
    return level


def centred(stream_key, extent, scale, bound, cuts=(), held_as=jnp.bfloat16):
    loudness = steps_of(stream_key, extent, cuts, -0.22, 0.18) if cuts else 1.0
    values = jax.random.normal(stream_key, extent, jnp.float32) * scale * loudness
    return jnp.minimum(jnp.maximum(values, -bound), bound).astype(held_as)


def bell_draw_with(stream_key, dims, scale, limit, shards, heavy, held_as=jnp.bfloat16):
    array = scale * jax.random.normal(stream_key, dims, jnp.float32)
    if shards:
        array = array * steps_of(stream_key, dims, shards, -0.22, 0.18)
    return jnp.clip(strengthened(array, jax.random.fold_in(stream_key, 3), *heavy), -limit, limit).astype(held_as)


def setup_inputs(seed: int = 0) -> dict:
    seeds = jax.random.split(jax.random.key(seed), 13)
    return {
        "q_latent": bell_draw_with(seeds[0], (TOKENS, LATENT), 1.0, 6.0, ((0, 8),), (0, 1, 8, 2.0)),
        "q_grad": centred(seeds[1], (TOKENS, QCOLS), 1.0, 6.0, ((0, 8), (1, 4))),
        "uq_master": centred(seeds[2], (LATENT, QCOLS), 1.0, 6.0, ((0, 8), (1, 4)), jnp.float32),
        "uq_basis": draw_uq_basis(jax.random.fold_in(seeds[12], 71), 0),
        "uq_first": centred(seeds[4], (RANK, QCOLS), 0.5, 3.0, ((0, 8), (1, 4)), jnp.float32),
        "uq_second": jnp.clip(jnp.exp(math.log(1.0) - 2.3025851 * jax.random.uniform(seeds[5], (RANK, QCOLS), jnp.float32) ** steps_of(seeds[5], (RANK, QCOLS), ((0, 8), (1, 4)), -0.2, 0.2)), 0.1, 1.0),
        "kv_latent": bell_draw_with(seeds[6], (TOKENS, LATENT), 1.0, 6.0, ((0, 8),), (0, 1, 8, 2.0)),
        "k_grad": centred(seeds[7], (TOKENS, KCOLS), 1.0, 6.0, ((0, 8), (1, 4))),
        "uk_master": centred(seeds[8], (LATENT, KCOLS), 1.0, 6.0, ((0, 8), (1, 4)), jnp.float32),
        "uk_basis": draw_uk_basis(jax.random.fold_in(seeds[12], 71), 0),
        "uk_first": centred(seeds[10], (RANK, KCOLS), 0.5, 3.0, ((0, 8), (1, 4)), jnp.float32),
        "uk_second": jnp.clip(jnp.exp(math.log(1.0) - 2.3025851 * jax.random.uniform(seeds[11], (RANK, KCOLS), jnp.float32) ** steps_of(seeds[11], (RANK, KCOLS), ((0, 8), (1, 4)), -0.2, 0.2)), 0.1, 1.0),
    }


first_decay = 0.8
second_decay = 0.9
step_size = 0.5
mean_guard = 1e-06
root_guard = 1e-08

def moment_update(scaled, first_old, second_old):
    first_new = first_decay * first_old + (1.0 - first_decay) * scaled
    second_new = second_decay * second_old + (1.0 - second_decay) * scaled * scaled
    heading = (first_new / (jnp.sqrt(second_new) + root_guard)).astype(jnp.bfloat16)
    return (first_new, second_new, heading)

def reference(q_latent, q_grad, uq_master, uq_basis, uq_first, uq_second, kv_latent, k_grad, uk_master, uk_basis, uk_first, uk_second):
    q_sum = jnp.dot(q_latent.T, q_grad, preferred_element_type=jnp.float32)
    k_sum = jnp.dot(kv_latent.T, k_grad, preferred_element_type=jnp.float32)
    q_proj = jnp.dot(uq_basis.astype(jnp.float32).T, q_sum, precision=lax.Precision.HIGHEST)
    k_proj = jnp.dot(uk_basis.astype(jnp.float32).T, k_sum, precision=lax.Precision.HIGHEST)
    squares_sum = jnp.sum(q_proj * q_proj) + jnp.sum(k_proj * k_proj)
    entry_count = q_proj.size + k_proj.size
    root_mean = jnp.sqrt(squares_sum / entry_count + mean_guard)
    uq_first_new, uq_second_new, q_dir = moment_update(q_proj / root_mean, uq_first, uq_second)
    uk_first_new, uk_second_new, k_dir = moment_update(k_proj / root_mean, uk_first, uk_second)
    uq_step = jnp.dot(uq_basis, q_dir, preferred_element_type=jnp.float32)
    uk_step = jnp.dot(uk_basis, k_dir, preferred_element_type=jnp.float32)
    uq_copy = (uq_master - step_size * uq_step).astype(jnp.bfloat16)
    uk_copy = (uk_master - step_size * uk_step).astype(jnp.bfloat16)
    return (uq_first_new, uq_second_new, uq_step, uq_copy, uk_first_new, uk_second_new, uk_step, uk_copy)
```

```python
import functools

import jax
import jax.numpy as jnp
from jax import lax
from jax.experimental import pallas as pl
from jax.experimental.pallas import tpu as pltpu
from jax.sharding import PartitionSpec as P

MESH = pl.DeviceIdType.MESH
F32 = jnp.float32
BF16 = jnp.bfloat16

first_decay = 0.8
second_decay = 0.9
step_size = 0.5
mean_guard = 1e-06
root_guard = 1e-08
PAIR = 2


def transposed_dot(left, right):
    return lax.dot_general(
        left, right, (((0,), (0,)), ((), ())), preferred_element_type=F32
    )


def exchange_kernel(
    n,
    tp_size,
    lq_hbm,
    gq_hbm,
    lk_hbm,
    gk_hbm,
    bq_hbm,
    bk_hbm,
    mq_hbm,
    mk_hbm,
    fq_hbm,
    sq_hbm,
    fk_hbm,
    sk_hbm,
    scaled_ref,
    dir_ref,
    master_ref,
    basis_ref,
    lq,
    gq,
    lk,
    gk,
    mq,
    mk,
    fq,
    sq,
    fk,
    sk,
    part_q,
    part_k,
    proj,
    px_out,
    px_in,
    pz_out,
    pz_in,
    st_out,
    st_in,
    sf_out,
    sf_in,
    local_sem,
    b_send,
    b_recv,
    m_send,
    m_recv,
    h_send,
    h_recv,
    px_send,
    px_recv,
    pz_send,
    pz_recv,
    st_send,
    st_recv,
    sf_send,
    sf_recv,
):
    outer = n // PAIR
    me = lax.axis_index("fs")
    tp = lax.axis_index("tp")
    z = me // PAIR
    x = lax.rem(me, PAIR)
    mate = z * PAIR + (1 - x)
    width_q = gq.shape[1]
    latent = n * basis_ref.shape[2]
    rank = basis_ref.shape[3]

    def level(i):
        return lax.rem(z + i, outer)

    def remote(src, dst, send, recv, fs_id, tp_id):
        return pltpu.make_async_remote_copy(
            src_ref=src,
            dst_ref=dst,
            send_sem=send,
            recv_sem=recv,
            device_id=(fs_id, tp_id),
            device_id_type=MESH,
        )

    loads = []
    for slot, (src, dst) in enumerate(
        (
            (bq_hbm, basis_ref.at[me, 0]),
            (bk_hbm, basis_ref.at[me, 1]),
            (mq_hbm, mq),
            (mk_hbm, mk),
            (lq_hbm, lq),
            (gq_hbm, gq),
            (lk_hbm, lk),
            (gk_hbm, gk),
            (fq_hbm, fq),
            (sq_hbm, sq),
            (fk_hbm, fk),
            (sk_hbm, sk),
        )
    ):
        copy = pltpu.make_async_copy(src, dst, local_sem.at[slot])
        copy.start()
        loads.append(copy)

    barrier = pltpu.get_barrier_semaphore()
    for i in range(1, n):
        pl.semaphore_signal(
            barrier, inc=1, device_id=(lax.rem(me + i, n), tp), device_id_type=MESH
        )
    for i in range(1, tp_size):
        pl.semaphore_signal(
            barrier, inc=1, device_id=(me, lax.rem(tp + i, tp_size)), device_id_type=MESH
        )
    pl.semaphore_wait(barrier, n - 1 + tp_size - 1)

    pending = []

    def send_own_along(buf, send, recv):
        for i in range(1, outer):
            copy = remote(
                buf.at[me], buf.at[me], send.at[i - 1], recv.at[me], level(i) * PAIR + x, tp
            )
            copy.start()
            pending.append(copy)

    def send_own_across(buf, send, recv):
        copy = remote(buf.at[me], buf.at[me], send.at[outer - 1], recv.at[me], mate, tp)
        copy.start()
        pending.append(copy)

    def forward_across(buf, send, recv, i):
        source = level(i) * PAIR + x
        copy = remote(
            buf.at[source], buf.at[source], send.at[outer - 1 + i], recv.at[source], mate, tp
        )
        copy.wait_recv()
        copy.start()
        pending.append(copy)

    def wait_across(buf, send, recv):
        for i in range(outer):
            source = level(i) * PAIR + (1 - x)
            remote(
                buf.at[source], buf.at[source], send.at[0], recv.at[source], mate, tp
            ).wait_recv()

    loads[0].wait()
    loads[1].wait()
    send_own_along(basis_ref, b_send, b_recv)
    send_own_across(basis_ref, b_send, b_recv)

    loads[2].wait()
    loads[3].wait()
    master_ref[me, :, :width_q] = mq[...].astype(BF16)
    master_ref[me, :, width_q:] = mk[...].astype(BF16)
    send_own_along(master_ref, m_send, m_recv)

    loads[4].wait()
    loads[5].wait()
    part_q[...] = transposed_dot(lq[...], gq[...])
    loads[6].wait()
    loads[7].wait()
    part_k[...] = transposed_dot(lk[...], gk[...])

    for i in range(1, outer):
        forward_across(basis_ref, b_send, b_recv, i)
    wait_across(basis_ref, b_send, b_recv)

    def project(which, partial):
        factor = basis_ref[:, which].reshape(latent, rank)
        high = partial.astype(BF16)
        low = (partial - high.astype(F32)).astype(BF16)
        return transposed_dot(factor, high) + transposed_dot(factor, low)

    rows = rank // n
    proj[:, :, :width_q] = project(0, part_q[...]).reshape(n, rows, width_q)
    proj[:, :, width_q:] = project(1, part_k[...]).reshape(n, rows, proj.shape[2] - width_q)

    order = [i for i in range(1, outer)] + [0]
    for i in order:
        zd = level(i)
        px_out[zd] = proj[zd * PAIR + (1 - x)].astype(BF16)
        copy = remote(px_out.at[zd], px_in.at[zd], px_send.at[zd], px_recv.at[zd], mate, tp)
        copy.start()
        pending.append(copy)
    send_own_across(master_ref, m_send, m_recv)

    def px_wait(zd):
        remote(
            px_out.at[zd], px_in.at[zd], px_send.at[zd], px_recv.at[zd], mate, tp
        ).wait_recv()

    for i in range(1, outer):
        zd = level(i)
        px_wait(zd)
        pz_out[zd] = (proj[zd * PAIR + x] + px_in[zd].astype(F32)).astype(BF16)
        copy = remote(
            pz_out.at[zd], pz_in.at[z], pz_send.at[zd], pz_recv.at[z], zd * PAIR + x, tp
        )
        copy.start()
        pending.append(copy)
    forward_across(master_ref, m_send, m_recv, 1)
    px_wait(z)
    total = proj[me] + px_in[z].astype(F32)
    for i in range(1, outer):
        zs = level(i)
        remote(
            pz_out.at[zs], pz_in.at[zs], pz_send.at[zs], pz_recv.at[zs], zs * PAIR + x, tp
        ).wait_recv()
        total = total + pz_in[zs].astype(F32)

    squares = jnp.full(st_out.shape, jnp.sum(total * total), F32)
    st_out[...] = squares
    for i in range(1, tp_size):
        copy = remote(
            st_out, st_in.at[tp], st_send.at[i], st_recv.at[tp], me, lax.rem(tp + i, tp_size)
        )
        copy.start()
        pending.append(copy)
    for i in range(1, tp_size):
        ts = lax.rem(tp + i, tp_size)
        remote(st_out, st_in.at[ts], st_send.at[i], st_recv.at[ts], me, ts).wait_recv()
        squares = squares + st_in[ts]
    sf_out[...] = squares
    for i in range(1, n):
        copy = remote(
            sf_out, sf_in.at[me], sf_send.at[i], sf_recv.at[me], lax.rem(me + i, n), tp
        )
        copy.start()
        pending.append(copy)
    for i in range(2, outer):
        forward_across(master_ref, m_send, m_recv, i)
    for i in range(1, n):
        fs = lax.rem(me + i, n)
        remote(sf_out, sf_in.at[fs], sf_send.at[i], sf_recv.at[fs], fs, tp).wait_recv()
        squares = squares + sf_in[fs]

    count = rows * proj.shape[2] * n * tp_size
    root_mean = jnp.sqrt(squares / count + mean_guard)[0:1, 0:1]
    scaled = total / root_mean
    scaled_ref[...] = scaled
    for load in loads[8:]:
        load.wait()
    dir_ref[me, :, :width_q] = moment_update(scaled[:, :width_q], fq[...], sq[...])[2]
    dir_ref[me, :, width_q:] = moment_update(scaled[:, width_q:], fk[...], sk[...])[2]
    send_own_along(dir_ref, h_send, h_recv)
    send_own_across(dir_ref, h_send, h_recv)
    for i in range(1, outer):
        forward_across(dir_ref, h_send, h_recv, i)
    wait_across(master_ref, m_send, m_recv)
    wait_across(dir_ref, h_send, h_recv)
    for copy in pending:
        copy.wait_send()


def apply_kernel(
    scaled_ref,
    dir_ref,
    master_ref,
    basis_ref,
    bq,
    bk,
    fq,
    sq,
    fk,
    sk,
    uq_first_new,
    uq_second_new,
    uq_step,
    uq_copy,
    uk_first_new,
    uk_second_new,
    uk_step,
    uk_copy,
):
    n, rows, width = dir_ref.shape
    deep = basis_ref.shape[2]
    rank = n * rows
    width_q = fq.shape[1]
    for which, cols, own, first, second, first_new, second_new, step, fresh in (
        (0, slice(0, width_q), bq, fq, sq, uq_first_new, uq_second_new, uq_step, uq_copy),
        (1, slice(width_q, width), bk, fk, sk, uk_first_new, uk_second_new, uk_step, uk_copy),
    ):
        span = cols.stop - cols.start
        moved = moment_update(scaled_ref[:, cols], first[...], second[...])
        first_new[...] = moved[0]
        second_new[...] = moved[1]
        heading = dir_ref[:, :, cols].reshape(rank, span)
        step[...] = jnp.dot(own[...], heading, preferred_element_type=F32)
        factor = basis_ref[:, which].reshape(n * deep, rank)
        whole = jnp.dot(factor, heading, preferred_element_type=F32)
        master = master_ref[:, :, cols].reshape(n * deep, span).astype(F32)
        fresh[...] = (master - step_size * whole).astype(BF16)


def kernel_body(
    n,
    tp_size,
    q_latent,
    q_grad,
    uq_master,
    uq_basis,
    uq_first,
    uq_second,
    kv_latent,
    k_grad,
    uk_master,
    uk_basis,
    uk_first,
    uk_second,
):
    outer = n // PAIR
    tokens, latent = q_latent.shape
    deep, rank = uq_basis.shape
    rows = rank // n
    width_q, width_k = q_grad.shape[1], k_grad.shape[1]
    width = width_q + width_k
    dma = pltpu.SemaphoreType.DMA
    vmem = pl.BlockSpec(memory_space=pltpu.VMEM)
    args = (
        q_latent, q_grad, kv_latent, k_grad, uq_basis, uk_basis,
        uq_master, uk_master, uq_first, uq_second, uk_first, uk_second,
    )
    scaled, heading, master, basis = pl.pallas_call(
        functools.partial(exchange_kernel, n, tp_size),
        out_shape=(
            jax.ShapeDtypeStruct((rows, width), F32),
            jax.ShapeDtypeStruct((n, rows, width), BF16),
            jax.ShapeDtypeStruct((n, deep, width), BF16),
            jax.ShapeDtypeStruct((n, 2, deep, rank), BF16),
        ),
        in_specs=[pl.BlockSpec(memory_space=pl.ANY)] * len(args),
        out_specs=(vmem,) * 4,
        scratch_shapes=[
            pltpu.VMEM(q_latent.shape, BF16),
            pltpu.VMEM(q_grad.shape, BF16),
            pltpu.VMEM(kv_latent.shape, BF16),
            pltpu.VMEM(k_grad.shape, BF16),
            pltpu.VMEM(uq_master.shape, F32),
            pltpu.VMEM(uk_master.shape, F32),
            pltpu.VMEM(uq_first.shape, F32),
            pltpu.VMEM(uq_second.shape, F32),
            pltpu.VMEM(uk_first.shape, F32),
            pltpu.VMEM(uk_second.shape, F32),
            pltpu.VMEM((latent, width_q), F32),
            pltpu.VMEM((latent, width_k), F32),
            pltpu.VMEM((n, rows, width), F32),
            pltpu.VMEM((outer, rows, width), BF16),
            pltpu.VMEM((outer, rows, width), BF16),
            pltpu.VMEM((outer, rows, width), BF16),
            pltpu.VMEM((outer, rows, width), BF16),
            pltpu.VMEM((8, 128), F32),
            pltpu.VMEM((tp_size, 8, 128), F32),
            pltpu.VMEM((8, 128), F32),
            pltpu.VMEM((n, 8, 128), F32),
            dma((len(args),)),
            dma((2 * outer - 1,)),
            dma((n,)),
            dma((2 * outer - 1,)),
            dma((n,)),
            dma((2 * outer - 1,)),
            dma((n,)),
            dma((outer,)),
            dma((outer,)),
            dma((outer,)),
            dma((outer,)),
            dma((tp_size,)),
            dma((tp_size,)),
            dma((n,)),
            dma((n,)),
        ],
        compiler_params=pltpu.CompilerParams(
            collective_id=0, has_side_effects=True, vmem_limit_bytes=40 * 1024 * 1024
        ),
        name="exchange",
    )(*args)
    shapes = tuple(
        jax.ShapeDtypeStruct(shape, dtype)
        for span in (width_q, width_k)
        for shape, dtype in (
            ((rows, span), F32),
            ((rows, span), F32),
            ((deep, span), F32),
            ((latent, span), BF16),
        )
    )
    return tuple(
        pl.pallas_call(
            apply_kernel,
            out_shape=shapes,
            in_specs=[vmem] * 10,
            out_specs=(vmem,) * 8,
            name="apply",
        )(
            scaled, heading, master, basis, uq_basis, uk_basis,
            uq_first, uq_second, uk_first, uk_second,
        )
    )


def across_tokens(left, right):
    return lax.dot_general(
        left, right, (((0,), (0,)), ((), ())), preferred_element_type=jnp.float32
    )


def across_latent(left, right):
    return lax.dot_general(
        left,
        right,
        (((0,), (0,)), ((), ())),
        precision=lax.Precision.HIGHEST,
        preferred_element_type=jnp.float32,
    )


def moment_update(scaled, first_old, second_old):
    first_new = first_decay * first_old + (1.0 - first_decay) * scaled
    second_new = second_decay * second_old + (1.0 - second_decay) * scaled * scaled
    heading = (first_new / (jnp.sqrt(second_new) + root_guard)).astype(jnp.bfloat16)
    return (first_new, second_new, heading)


def body(
    q_latent,
    q_grad,
    uq_master,
    uq_basis,
    uq_first,
    uq_second,
    kv_latent,
    k_grad,
    uk_master,
    uk_basis,
    uk_first,
    uk_second,
):
    q_width = q_grad.shape[1]
    q_whole, k_whole = (
        lax.all_gather(uq_basis, "fs", axis=0, tiled=True),
        lax.all_gather(uk_basis, "fs", axis=0, tiled=True),
    )
    q_factor = q_whole.astype(jnp.float32)
    k_factor = k_whole.astype(jnp.float32)
    q_partial = across_tokens(q_latent, q_grad)
    k_partial = across_tokens(kv_latent, k_grad)
    projected = lax.psum_scatter(
        jnp.concatenate(
            [across_latent(q_factor, q_partial), across_latent(k_factor, k_partial)], axis=1
        ),
        "fs",
        scatter_dimension=0,
        tiled=True,
    )
    squares_sum = lax.psum(jnp.sum(projected * projected), ("fs", "tp"))
    entry_count = (
        projected.shape[0] * projected.shape[1] * lax.axis_size("fs") * lax.axis_size("tp")
    )
    root_mean = jnp.sqrt(squares_sum / entry_count + mean_guard)
    scaled = projected / root_mean
    uq_first_new, uq_second_new, q_heading = moment_update(scaled[:, :q_width], uq_first, uq_second)
    uk_first_new, uk_second_new, k_heading = moment_update(scaled[:, q_width:], uk_first, uk_second)
    q_dir, k_dir = (
        lax.all_gather(q_heading, "fs", axis=0, tiled=True),
        lax.all_gather(k_heading, "fs", axis=0, tiled=True),
    )
    uq_step = jnp.dot(uq_basis, q_dir, preferred_element_type=jnp.float32)
    uk_step = jnp.dot(uk_basis, k_dir, preferred_element_type=jnp.float32)
    q_fresh = (uq_master - step_size * uq_step).astype(jnp.bfloat16)
    k_fresh = (uk_master - step_size * uk_step).astype(jnp.bfloat16)
    uq_copy, uk_copy = (
        lax.all_gather(q_fresh, "fs", axis=0, tiled=True),
        lax.all_gather(k_fresh, "fs", axis=0, tiled=True),
    )
    return (
        uq_first_new,
        uq_second_new,
        uq_step,
        uq_copy,
        uk_first_new,
        uk_second_new,
        uk_step,
        uk_copy,
    )


def chosen_body(n, tp_size, *args):
    deep, rank = args[3].shape
    tiled = n % PAIR == 0 and rank % (16 * n) == 0 and deep % 16 == 0
    lanes = args[1].shape[1] % 128 == 0 and args[7].shape[1] % 128 == 0 and rank % 128 == 0
    if tiled and lanes:
        return kernel_body(n, tp_size, *args)
    return body(*args)


def solution(mesh):
    return jax.shard_map(
        functools.partial(chosen_body, mesh.shape["fs"], mesh.shape["tp"]),
        mesh=mesh,
        in_specs=(
            P("fs", None),
            P("fs", "tp"),
            P("fs", "tp"),
            P("fs", None),
            P("fs", "tp"),
            P("fs", "tp"),
            P("fs", None),
            P("fs", "tp"),
            P("fs", "tp"),
            P("fs", None),
            P("fs", "tp"),
            P("fs", "tp"),
        ),
        out_specs=(
            P("fs", "tp"),
            P("fs", "tp"),
            P("fs", "tp"),
            P(None, "tp"),
            P("fs", "tp"),
            P("fs", "tp"),
            P("fs", "tp"),
            P(None, "tp"),
        ),
        check_vma=False,
    )
```

```python
import functools

import jax
import jax.numpy as jnp
from jax import lax
from jax.experimental import pallas as pl
from jax.experimental.pallas import tpu as pltpu
from jax.sharding import PartitionSpec as P

MESH = pl.DeviceIdType.MESH
F32 = jnp.float32
BF16 = jnp.bfloat16

first_decay = 0.8
second_decay = 0.9
step_size = 0.5
mean_guard = 1e-06
root_guard = 1e-08
PAIR = 2
VMEM_BYTES = 67043328


def transposed_dot(left, right):
    return lax.dot_general(
        left, right, (((0,), (0,)), ((), ())), preferred_element_type=F32
    )


def exchange_kernel(
    n,
    tp_size,
    lq_hbm,
    gq_hbm,
    lk_hbm,
    gk_hbm,
    bq_hbm,
    bk_hbm,
    mq_hbm,
    mk_hbm,
    fq_hbm,
    sq_hbm,
    fk_hbm,
    sk_hbm,
    scaled_out,
    dir_out,
    master_out,
    basis_out,
    scaled_ref,
    dir_ref,
    master_ref,
    basis_ref,
    lq,
    gq,
    lk,
    gk,
    mq,
    mk,
    fq,
    sq,
    fk,
    sk,
    part_q,
    part_k,
    proj,
    px_out,
    px_in,
    pz_out,
    pz_in,
    st_out,
    st_in,
    sf_out,
    sf_in,
    local_sem,
    out_sem,
    dir_sem,
    b_send,
    b_recv,
    c_send,
    c_recv,
    m_send,
    m_recv,
    h_send,
    h_recv,
    px_send,
    px_recv,
    pz_send,
    pz_recv,
    st_send,
    st_recv,
    sf_send,
    sf_recv,
):
    outer = n // PAIR
    me = lax.axis_index("fs")
    tp = lax.axis_index("tp")
    z = me // PAIR
    x = lax.rem(me, PAIR)
    mate = z * PAIR + (1 - x)
    which = lax.rem(tp, PAIR)
    twin = tp + 1 - 2 * which
    width_q = gq.shape[1]
    latent = n * basis_ref.shape[2]
    rank = basis_ref.shape[3]

    def level(i):
        return lax.rem(z + i, outer)

    def remote(src, dst, send, recv, fs_id, tp_id):
        return pltpu.make_async_remote_copy(
            src_ref=src,
            dst_ref=dst,
            send_sem=send,
            recv_sem=recv,
            device_id=(fs_id, tp_id),
            device_id_type=MESH,
        )

    loads = []
    for slot, (src, dst) in enumerate(
        (
            (bq_hbm, basis_ref.at[me, 0]),
            (bk_hbm, basis_ref.at[me, 1]),
            (mq_hbm, mq),
            (mk_hbm, mk),
            (lq_hbm, lq),
            (gq_hbm, gq),
            (lk_hbm, lk),
            (gk_hbm, gk),
            (fq_hbm, fq),
            (sq_hbm, sq),
            (fk_hbm, fk),
            (sk_hbm, sk),
        )
    ):
        copy = pltpu.make_async_copy(src, dst, local_sem.at[slot])
        copy.start()
        loads.append(copy)

    barrier = pltpu.get_barrier_semaphore()
    for i in range(1, n):
        pl.semaphore_signal(
            barrier, inc=1, device_id=(lax.rem(me + i, n), tp), device_id_type=MESH
        )
    for i in range(1, tp_size):
        pl.semaphore_signal(
            barrier, inc=1, device_id=(me, lax.rem(tp + i, tp_size)), device_id_type=MESH
        )
    pl.semaphore_wait(barrier, n - 1 + tp_size - 1)

    pending = []

    def start(copy, when=None):
        if when is None:
            copy.start()
        else:
            pl.when(when)(copy.start)
        pending.append((copy, when))

    def send_out(src, dst, sem):
        copy = pltpu.make_async_copy(src, dst, sem)
        copy.start()
        stores.append(copy)

    stores = []

    def basis_copy(source, send, fs_id):
        slot = basis_ref.at[source, which]
        return remote(slot, slot, b_send.at[send], b_recv.at[source], fs_id, tp)

    def to_twin(source):
        slot = basis_ref.at[source, which]
        start(remote(slot, slot, c_send.at[source], c_recv.at[source], me, twin))

    loads[0].wait()
    loads[1].wait()
    for i in range(1, outer):
        start(basis_copy(me, i - 1, level(i) * PAIR + x))
    start(basis_copy(me, outer - 1, mate))

    loads[2].wait()
    loads[3].wait()
    master_ref[me, :, :width_q] = mq[...].astype(BF16)
    master_ref[me, :, width_q:] = mk[...].astype(BF16)

    def master_copy(source, send, fs_id):
        slot = master_ref.at[source]
        return remote(slot, slot, m_send.at[send], m_recv.at[source], fs_id, tp)

    def toward(sign, hop):
        holds = (z >= hop) if sign > 0 else (z + hop < outer)
        room = (z + 1 < outer) if sign > 0 else (z >= 1)
        near = level(outer + sign) * PAIR + x
        source = level(outer - sign * hop) * PAIR + x
        return holds, room, near, source

    def send_master_along(hop):
        for side, sign in enumerate((1, -1)):
            holds, room, near, source = toward(sign, hop)
            if hop:
                copy = master_copy(source, 0, near)
                pl.when(holds)(copy.wait_recv)
            if hop < outer - 1:
                copy = master_copy(source, 2 * hop + side, near)
                start(copy, jnp.logical_and(holds, room) if hop else room)

    def send_master_across(hop):
        base = 2 * (outer - 1)
        if hop == 0:
            start(master_copy(me, base, mate))
            return
        for side, sign in enumerate((1, -1)):
            holds, _, _, source = toward(sign, hop)
            start(master_copy(source, base + 2 * hop - 1 + side, mate), holds)

    send_master_along(0)

    loads[4].wait()
    loads[5].wait()
    part_q[...] = transposed_dot(lq[...], gq[...])
    loads[6].wait()
    loads[7].wait()
    part_k[...] = transposed_dot(lk[...], gk[...])

    for i in range(1, outer):
        source = level(i) * PAIR + x
        copy = basis_copy(source, outer - 1 + i, mate)
        copy.wait_recv()
        start(copy)
        to_twin(source)
    send_master_across(0)
    for i in range(outer):
        source = level(i) * PAIR + (1 - x)
        basis_copy(source, 0, mate).wait_recv()
        to_twin(source)
    for i in range(1, n):
        source = lax.rem(me + i, n)
        slot = basis_ref.at[source, 1 - which]
        remote(slot, slot, c_send.at[source], c_recv.at[source], me, twin).wait_recv()
    send_out(basis_ref, basis_out, out_sem.at[0])

    def project(side, partial):
        factor = basis_ref[:, side].reshape(latent, rank)
        high = partial.astype(BF16)
        low = (partial - high.astype(F32)).astype(BF16)
        return transposed_dot(factor, high) + transposed_dot(factor, low)

    rows = rank // n
    proj[:, :, :width_q] = project(0, part_q[...]).reshape(n, rows, width_q)
    proj[:, :, width_q:] = project(1, part_k[...]).reshape(n, rows, proj.shape[2] - width_q)

    order = [i for i in range(1, outer)] + [0]
    for i in order:
        zd = level(i)
        px_out[zd] = proj[zd * PAIR + (1 - x)].astype(BF16)
        start(remote(px_out.at[zd], px_in.at[zd], px_send.at[zd], px_recv.at[zd], mate, tp))
        if i == 1:
            send_master_along(1)
    send_master_across(1)

    def px_wait(zd):
        remote(
            px_out.at[zd], px_in.at[zd], px_send.at[zd], px_recv.at[zd], mate, tp
        ).wait_recv()

    for i in range(1, outer):
        zd = level(i)
        px_wait(zd)
        pz_out[zd] = (proj[zd * PAIR + x] + px_in[zd].astype(F32)).astype(BF16)
        start(
            remote(pz_out.at[zd], pz_in.at[z], pz_send.at[zd], pz_recv.at[z], zd * PAIR + x, tp)
        )
        if i == 1:
            for hop in range(2, outer - 1):
                send_master_along(hop)
    for hop in range(2, outer - 1):
        send_master_across(hop)
    px_wait(z)
    total = proj[me] + px_in[z].astype(F32)
    for i in range(1, outer):
        zs = level(i)
        remote(
            pz_out.at[zs], pz_in.at[zs], pz_send.at[zs], pz_recv.at[zs], zs * PAIR + x, tp
        ).wait_recv()
        total = total + pz_in[zs].astype(F32)

    squares = jnp.full(st_out.shape, jnp.sum(total * total), F32)
    st_out[...] = squares
    for i in range(1, tp_size):
        start(
            remote(
                st_out, st_in.at[tp], st_send.at[i], st_recv.at[tp], me, lax.rem(tp + i, tp_size)
            )
        )
    for i in range(1, tp_size):
        ts = lax.rem(tp + i, tp_size)
        remote(st_out, st_in.at[ts], st_send.at[i], st_recv.at[ts], me, ts).wait_recv()
        squares = squares + st_in[ts]
    sf_out[...] = squares
    for i in range(1, n):
        start(
            remote(sf_out, sf_in.at[me], sf_send.at[i], sf_recv.at[me], lax.rem(me + i, n), tp)
        )
    send_master_along(outer - 1)
    send_master_across(outer - 1)
    for i in range(1, n):
        fs = lax.rem(me + i, n)
        remote(sf_out, sf_in.at[fs], sf_send.at[i], sf_recv.at[fs], fs, tp).wait_recv()
        squares = squares + sf_in[fs]

    count = rows * proj.shape[2] * n * tp_size
    root_mean = jnp.sqrt(squares / count + mean_guard)[0:1, 0:1]
    scaled = total / root_mean
    scaled_ref[...] = scaled
    for load in loads[8:]:
        load.wait()
    dir_ref[me, :, :width_q] = moment_update(scaled[:, :width_q], fq[...], sq[...])[2]
    dir_ref[me, :, width_q:] = moment_update(scaled[:, width_q:], fk[...], sk[...])[2]
    def dir_copy(source, send, fs_id):
        slot = dir_ref.at[source]
        return remote(slot, slot, h_send.at[send], h_recv.at[source], fs_id, tp)

    def dir_store(source):
        send_out(dir_ref.at[source], dir_out.at[source], dir_sem.at[source])

    for i in range(1, outer):
        start(dir_copy(me, i - 1, level(i) * PAIR + x))
    start(dir_copy(me, outer - 1, mate))
    send_out(scaled_ref, scaled_out, out_sem.at[1])
    dir_store(me)
    for i in range(outer):
        source = level(i) * PAIR + (1 - x)
        master_copy(source, 0, mate).wait_recv()
    send_out(master_ref, master_out, out_sem.at[2])
    for i in range(1, outer):
        source = level(i) * PAIR + x
        copy = dir_copy(source, outer - 1 + i, mate)
        copy.wait_recv()
        start(copy)
        dir_store(source)
    for i in range(outer):
        source = level(i) * PAIR + (1 - x)
        dir_copy(source, 0, mate).wait_recv()
        dir_store(source)
    for copy, when in pending:
        if when is None:
            copy.wait_send()
        else:
            pl.when(when)(copy.wait_send)
    for copy in stores:
        copy.wait()


def apply_kernel(
    scaled_ref,
    dir_ref,
    master_ref,
    basis_ref,
    bq,
    bk,
    fq,
    sq,
    fk,
    sk,
    uq_first_new,
    uq_second_new,
    uq_step,
    uq_copy,
    uk_first_new,
    uk_second_new,
    uk_step,
    uk_copy,
):
    n, rows, width = dir_ref.shape
    deep = basis_ref.shape[2]
    rank = n * rows
    width_q = fq.shape[1]
    for which, cols, own, first, second, first_new, second_new, step, fresh in (
        (0, slice(0, width_q), bq, fq, sq, uq_first_new, uq_second_new, uq_step, uq_copy),
        (1, slice(width_q, width), bk, fk, sk, uk_first_new, uk_second_new, uk_step, uk_copy),
    ):
        span = cols.stop - cols.start
        moved = moment_update(scaled_ref[:, cols], first[...], second[...])
        first_new[...] = moved[0]
        second_new[...] = moved[1]
        heading = dir_ref[:, :, cols].reshape(rank, span)
        step[...] = jnp.dot(own[...], heading, preferred_element_type=F32)
        factor = basis_ref[:, which].reshape(n * deep, rank)
        whole = jnp.dot(factor, heading, preferred_element_type=F32)
        master = master_ref[:, :, cols].reshape(n * deep, span).astype(F32)
        fresh[...] = (master - step_size * whole).astype(BF16)


def kernel_body(
    n,
    tp_size,
    q_latent,
    q_grad,
    uq_master,
    uq_basis,
    uq_first,
    uq_second,
    kv_latent,
    k_grad,
    uk_master,
    uk_basis,
    uk_first,
    uk_second,
):
    outer = n // PAIR
    tokens, latent = q_latent.shape
    deep, rank = uq_basis.shape
    rows = rank // n
    width_q, width_k = q_grad.shape[1], k_grad.shape[1]
    width = width_q + width_k
    dma = pltpu.SemaphoreType.DMA
    vmem = pl.BlockSpec(memory_space=pltpu.VMEM)
    args = (
        q_latent, q_grad, kv_latent, k_grad, uq_basis, uk_basis,
        uq_master, uk_master, uq_first, uq_second, uk_first, uk_second,
    )
    scaled, heading, master, basis = pl.pallas_call(
        functools.partial(exchange_kernel, n, tp_size),
        out_shape=(
            jax.ShapeDtypeStruct((rows, width), F32),
            jax.ShapeDtypeStruct((n, rows, width), BF16),
            jax.ShapeDtypeStruct((n, deep, width), BF16),
            jax.ShapeDtypeStruct((n, 2, deep, rank), BF16),
        ),
        in_specs=[pl.BlockSpec(memory_space=pl.ANY)] * len(args),
        out_specs=(pl.BlockSpec(memory_space=pl.ANY),) * 4,
        scratch_shapes=[
            pltpu.VMEM((rows, width), F32),
            pltpu.VMEM((n, rows, width), BF16),
            pltpu.VMEM((n, deep, width), BF16),
            pltpu.VMEM((n, 2, deep, rank), BF16),
            pltpu.VMEM(q_latent.shape, BF16),
            pltpu.VMEM(q_grad.shape, BF16),
            pltpu.VMEM(kv_latent.shape, BF16),
            pltpu.VMEM(k_grad.shape, BF16),
            pltpu.VMEM(uq_master.shape, F32),
            pltpu.VMEM(uk_master.shape, F32),
            pltpu.VMEM(uq_first.shape, F32),
            pltpu.VMEM(uq_second.shape, F32),
            pltpu.VMEM(uk_first.shape, F32),
            pltpu.VMEM(uk_second.shape, F32),
            pltpu.VMEM((latent, width_q), F32),
            pltpu.VMEM((latent, width_k), F32),
            pltpu.VMEM((n, rows, width), F32),
            pltpu.VMEM((outer, rows, width), BF16),
            pltpu.VMEM((outer, rows, width), BF16),
            pltpu.VMEM((outer, rows, width), BF16),
            pltpu.VMEM((outer, rows, width), BF16),
            pltpu.VMEM((8, 128), F32),
            pltpu.VMEM((tp_size, 8, 128), F32),
            pltpu.VMEM((8, 128), F32),
            pltpu.VMEM((n, 8, 128), F32),
            dma((len(args),)),
            dma((3,)),
            dma((n,)),
            dma((2 * outer - 1,)),
            dma((n,)),
            dma((n,)),
            dma((n,)),
            dma((4 * outer - 3,)),
            dma((n,)),
            dma((2 * outer - 1,)),
            dma((n,)),
            dma((outer,)),
            dma((outer,)),
            dma((outer,)),
            dma((outer,)),
            dma((tp_size,)),
            dma((tp_size,)),
            dma((n,)),
            dma((n,)),
        ],
        compiler_params=pltpu.CompilerParams(
            collective_id=0, has_side_effects=True, vmem_limit_bytes=VMEM_BYTES
        ),
        name="exchange",
    )(*args)
    shapes = tuple(
        jax.ShapeDtypeStruct(shape, dtype)
        for span in (width_q, width_k)
        for shape, dtype in (
            ((rows, span), F32),
            ((rows, span), F32),
            ((deep, span), F32),
            ((latent, span), BF16),
        )
    )
    return tuple(
        pl.pallas_call(
            apply_kernel,
            out_shape=shapes,
            in_specs=[vmem] * 10,
            out_specs=(vmem,) * 8,
            name="apply",
        )(
            scaled, heading, master, basis, uq_basis, uk_basis,
            uq_first, uq_second, uk_first, uk_second,
        )
    )


def across_tokens(left, right):
    return lax.dot_general(
        left, right, (((0,), (0,)), ((), ())), preferred_element_type=jnp.float32
    )


def across_latent(left, right):
    return lax.dot_general(
        left,
        right,
        (((0,), (0,)), ((), ())),
        precision=lax.Precision.HIGHEST,
        preferred_element_type=jnp.float32,
    )


def moment_update(scaled, first_old, second_old):
    first_new = first_decay * first_old + (1.0 - first_decay) * scaled
    second_new = second_decay * second_old + (1.0 - second_decay) * scaled * scaled
    heading = (first_new / (jnp.sqrt(second_new) + root_guard)).astype(jnp.bfloat16)
    return (first_new, second_new, heading)


def body(
    q_latent,
    q_grad,
    uq_master,
    uq_basis,
    uq_first,
    uq_second,
    kv_latent,
    k_grad,
    uk_master,
    uk_basis,
    uk_first,
    uk_second,
):
    q_width = q_grad.shape[1]
    q_whole, k_whole = (
        lax.all_gather(uq_basis, "fs", axis=0, tiled=True),
        lax.all_gather(uk_basis, "fs", axis=0, tiled=True),
    )
    q_factor = q_whole.astype(jnp.float32)
    k_factor = k_whole.astype(jnp.float32)
    q_partial = across_tokens(q_latent, q_grad)
    k_partial = across_tokens(kv_latent, k_grad)
    projected = lax.psum_scatter(
        jnp.concatenate(
            [across_latent(q_factor, q_partial), across_latent(k_factor, k_partial)], axis=1
        ),
        "fs",
        scatter_dimension=0,
        tiled=True,
    )
    squares_sum = lax.psum(jnp.sum(projected * projected), ("fs", "tp"))
    entry_count = (
        projected.shape[0] * projected.shape[1] * lax.axis_size("fs") * lax.axis_size("tp")
    )
    root_mean = jnp.sqrt(squares_sum / entry_count + mean_guard)
    scaled = projected / root_mean
    uq_first_new, uq_second_new, q_heading = moment_update(scaled[:, :q_width], uq_first, uq_second)
    uk_first_new, uk_second_new, k_heading = moment_update(scaled[:, q_width:], uk_first, uk_second)
    q_dir, k_dir = (
        lax.all_gather(q_heading, "fs", axis=0, tiled=True),
        lax.all_gather(k_heading, "fs", axis=0, tiled=True),
    )
    uq_step = jnp.dot(uq_basis, q_dir, preferred_element_type=jnp.float32)
    uk_step = jnp.dot(uk_basis, k_dir, preferred_element_type=jnp.float32)
    q_fresh = (uq_master - step_size * uq_step).astype(jnp.bfloat16)
    k_fresh = (uk_master - step_size * uk_step).astype(jnp.bfloat16)
    uq_copy, uk_copy = (
        lax.all_gather(q_fresh, "fs", axis=0, tiled=True),
        lax.all_gather(k_fresh, "fs", axis=0, tiled=True),
    )
    return (
        uq_first_new,
        uq_second_new,
        uq_step,
        uq_copy,
        uk_first_new,
        uk_second_new,
        uk_step,
        uk_copy,
    )


def chosen_body(n, tp_size, *args):
    deep, rank = args[3].shape
    tiled = n > 2 * PAIR and n % PAIR == 0 and tp_size % PAIR == 0 and rank % (16 * n) == 0 and deep % 16 == 0
    lanes = args[1].shape[1] % 128 == 0 and args[7].shape[1] % 128 == 0 and rank % 128 == 0
    if tiled and lanes:
        return kernel_body(n, tp_size, *args)
    return body(*args)


def solution(mesh):
    return jax.shard_map(
        functools.partial(chosen_body, mesh.shape["fs"], mesh.shape["tp"]),
        mesh=mesh,
        in_specs=(
            P("fs", None),
            P("fs", "tp"),
            P("fs", "tp"),
            P("fs", None),
            P("fs", "tp"),
            P("fs", "tp"),
            P("fs", None),
            P("fs", "tp"),
            P("fs", "tp"),
            P("fs", None),
            P("fs", "tp"),
            P("fs", "tp"),
        ),
        out_specs=(
            P("fs", "tp"),
            P("fs", "tp"),
            P("fs", "tp"),
            P(None, "tp"),
            P("fs", "tp"),
            P("fs", "tp"),
            P("fs", "tp"),
            P(None, "tp"),
        ),
        check_vma=False,
    )
```

```python
import functools

import jax
import jax.numpy as jnp
from jax import lax
from jax.experimental import pallas as pl
from jax.experimental.pallas import tpu as pltpu
from jax.sharding import PartitionSpec as P

MESH = pl.DeviceIdType.MESH
F32 = jnp.float32
BF16 = jnp.bfloat16

first_decay = 0.8
second_decay = 0.9
step_size = 0.5
mean_guard = 1e-06
root_guard = 1e-08
PAIR = 2
VMEM_BYTES = 67043328


def transposed_dot(left, right):
    return lax.dot_general(
        left, right, (((0,), (0,)), ((), ())), preferred_element_type=F32
    )


def exchange_kernel(
    n,
    tp_size,
    lq_hbm,
    gq_hbm,
    lk_hbm,
    gk_hbm,
    bq_hbm,
    bk_hbm,
    mq_hbm,
    mk_hbm,
    fq_hbm,
    sq_hbm,
    fk_hbm,
    sk_hbm,
    scaled_out,
    dir_out,
    master_out,
    basis_out,
    scaled_ref,
    dir_ref,
    master_ref,
    basis_ref,
    lq,
    gq,
    lk,
    gk,
    mq,
    mk,
    fq,
    sq,
    fk,
    sk,
    part_q,
    part_k,
    proj,
    px_out,
    px_in,
    pz_out,
    pz_in,
    st_out,
    st_in,
    sf_out,
    sf_in,
    local_sem,
    out_sem,
    dir_sem,
    b_send,
    b_recv,
    c_send,
    c_recv,
    m_send,
    m_recv,
    h_send,
    h_recv,
    px_send,
    px_recv,
    pz_send,
    pz_recv,
    st_send,
    st_recv,
    sf_send,
    sf_recv,
):
    outer = n // PAIR
    me = lax.axis_index("fs")
    tp = lax.axis_index("tp")
    z = me // PAIR
    x = lax.rem(me, PAIR)
    mate = z * PAIR + (1 - x)
    which = lax.rem(tp, PAIR)
    twin = tp + 1 - 2 * which
    width_q = gq.shape[1]
    latent = n * basis_ref.shape[2]
    rank = basis_ref.shape[3]

    def level(i):
        return lax.rem(z + i, outer)

    def remote(src, dst, send, recv, fs_id, tp_id):
        return pltpu.make_async_remote_copy(
            src_ref=src,
            dst_ref=dst,
            send_sem=send,
            recv_sem=recv,
            device_id=(fs_id, tp_id),
            device_id_type=MESH,
        )

    loads = []
    for slot, (src, dst) in enumerate(
        (
            (bq_hbm, basis_ref.at[me, 0]),
            (bk_hbm, basis_ref.at[me, 1]),
            (mq_hbm, mq),
            (mk_hbm, mk),
            (lq_hbm, lq),
            (gq_hbm, gq),
            (lk_hbm, lk),
            (gk_hbm, gk),
            (fq_hbm, fq),
            (sq_hbm, sq),
            (fk_hbm, fk),
            (sk_hbm, sk),
        )
    ):
        copy = pltpu.make_async_copy(src, dst, local_sem.at[slot])
        copy.start()
        loads.append(copy)

    barrier = pltpu.get_barrier_semaphore()
    for i in range(1, n):
        pl.semaphore_signal(
            barrier, inc=1, device_id=(lax.rem(me + i, n), tp), device_id_type=MESH
        )
    for i in range(1, tp_size):
        pl.semaphore_signal(
            barrier, inc=1, device_id=(me, lax.rem(tp + i, tp_size)), device_id_type=MESH
        )
    pl.semaphore_wait(barrier, n - 1 + tp_size - 1)

    pending = []

    def start(copy, when=None):
        if when is None:
            copy.start()
        else:
            pl.when(when)(copy.start)
        pending.append((copy, when))

    def send_out(src, dst, sem):
        copy = pltpu.make_async_copy(src, dst, sem)
        copy.start()
        stores.append(copy)

    stores = []

    def basis_copy(source, send, fs_id):
        slot = basis_ref.at[source, which]
        return remote(slot, slot, b_send.at[send], b_recv.at[source], fs_id, tp)

    def to_twin(source):
        slot = basis_ref.at[source, which]
        start(remote(slot, slot, c_send.at[source], c_recv.at[source], me, twin))

    loads[0].wait()
    loads[1].wait()
    for i in range(1, outer):
        start(basis_copy(me, i - 1, level(i) * PAIR + x))
    start(basis_copy(me, outer - 1, mate))

    loads[2].wait()
    loads[3].wait()
    master_ref[me, :, :width_q] = mq[...].astype(BF16)
    master_ref[me, :, width_q:] = mk[...].astype(BF16)

    def master_copy(source, send, fs_id):
        slot = master_ref.at[source]
        return remote(slot, slot, m_send.at[send], m_recv.at[source], fs_id, tp)

    def toward(sign, hop):
        holds = (z >= hop) if sign > 0 else (z + hop < outer)
        room = (z + 1 < outer) if sign > 0 else (z >= 1)
        near = level(outer + sign) * PAIR + x
        source = level(outer - sign * hop) * PAIR + x
        return holds, room, near, source

    def send_master_along(hop):
        for side, sign in enumerate((1, -1)):
            holds, room, near, source = toward(sign, hop)
            if hop:
                copy = master_copy(source, 0, near)
                pl.when(holds)(copy.wait_recv)
            if hop < outer - 1:
                copy = master_copy(source, 2 * hop + side, near)
                start(copy, jnp.logical_and(holds, room) if hop else room)

    def send_master_across(hop):
        base = 2 * (outer - 1)
        if hop == 0:
            start(master_copy(me, base, mate))
            return
        for side, sign in enumerate((1, -1)):
            holds, _, _, source = toward(sign, hop)
            start(master_copy(source, base + 2 * hop - 1 + side, mate), holds)

    send_master_along(0)

    loads[4].wait()
    loads[5].wait()
    part_q[...] = transposed_dot(lq[...], gq[...])
    loads[6].wait()
    loads[7].wait()
    part_k[...] = transposed_dot(lk[...], gk[...])

    for i in range(1, outer):
        source = level(i) * PAIR + x
        copy = basis_copy(source, outer - 1 + i, mate)
        copy.wait_recv()
        start(copy)
        to_twin(source)
    send_master_across(0)
    for i in range(outer):
        source = level(i) * PAIR + (1 - x)
        basis_copy(source, 0, mate).wait_recv()
        to_twin(source)
    for i in range(1, n):
        source = lax.rem(me + i, n)
        slot = basis_ref.at[source, 1 - which]
        remote(slot, slot, c_send.at[source], c_recv.at[source], me, twin).wait_recv()
    send_out(basis_ref, basis_out, out_sem.at[0])

    def project(side, partial):
        factor = basis_ref[:, side].reshape(latent, rank)
        high = partial.astype(BF16)
        low = (partial - high.astype(F32)).astype(BF16)
        return transposed_dot(factor, high) + transposed_dot(factor, low)

    rows = rank // n
    width = proj.shape[2]
    pieces = (slice(0, width_q), slice(width_q, width))
    partials = (part_q, part_k)

    def px_copy(zd, side):
        cols = pieces[side]
        return remote(
            px_out.at[zd, :, cols],
            px_in.at[zd, :, cols],
            px_send.at[zd, side],
            px_recv.at[zd, side],
            mate,
            tp,
        )

    def pz_copy(zd, zs, side):
        cols = pieces[side]
        return remote(
            pz_out.at[zd, :, cols],
            pz_in.at[zs, :, cols],
            pz_send.at[zd, side],
            pz_recv.at[zs, side],
            zd * PAIR + x,
            tp,
        )

    order = [i for i in range(1, outer)] + [0]
    for side, cols in enumerate(pieces):
        span = cols.stop - cols.start
        proj[:, :, cols] = project(side, partials[side][...]).reshape(n, rows, span)
        for i in order:
            zd = level(i)
            px_out[zd, :, cols] = proj[zd * PAIR + (1 - x), :, cols].astype(BF16)
            start(px_copy(zd, side))
    send_master_along(1)
    send_master_across(1)

    for side, cols in enumerate(pieces):
        for i in range(1, outer):
            zd = level(i)
            px_copy(zd, side).wait_recv()
            pz_out[zd, :, cols] = (
                proj[zd * PAIR + x, :, cols] + px_in[zd, :, cols].astype(F32)
            ).astype(BF16)
            start(pz_copy(zd, z, side))
        px_copy(z, side).wait_recv()
    for hop in range(2, outer - 1):
        send_master_along(hop)
    total = proj[me] + px_in[z].astype(F32)
    for i in range(1, outer):
        zs = level(i)
        for side in range(len(pieces)):
            pz_copy(zs, zs, side).wait_recv()
        total = total + pz_in[zs].astype(F32)

    squares = jnp.full(st_out.shape, jnp.sum(total * total), F32)
    st_out[...] = squares
    for i in range(1, tp_size):
        start(
            remote(
                st_out, st_in.at[tp], st_send.at[i], st_recv.at[tp], me, lax.rem(tp + i, tp_size)
            )
        )
    for i in range(1, tp_size):
        ts = lax.rem(tp + i, tp_size)
        remote(st_out, st_in.at[ts], st_send.at[i], st_recv.at[ts], me, ts).wait_recv()
        squares = squares + st_in[ts]
    sf_out[...] = squares
    for i in range(1, n):
        start(
            remote(sf_out, sf_in.at[me], sf_send.at[i], sf_recv.at[me], lax.rem(me + i, n), tp)
        )
    for hop in range(2, outer - 1):
        send_master_across(hop)
    send_master_along(outer - 1)
    send_master_across(outer - 1)
    for i in range(1, n):
        fs = lax.rem(me + i, n)
        remote(sf_out, sf_in.at[fs], sf_send.at[i], sf_recv.at[fs], fs, tp).wait_recv()
        squares = squares + sf_in[fs]

    count = rows * width * n * tp_size
    root_mean = jnp.sqrt(squares / count + mean_guard)[0:1, 0:1]
    scaled = total / root_mean
    scaled_ref[...] = scaled
    for load in loads[8:]:
        load.wait()
    def dir_copy(source, send, fs_id, side):
        slot = dir_ref.at[source, :, pieces[side]]
        return remote(slot, slot, h_send.at[send, side], h_recv.at[source, side], fs_id, tp)

    def dir_store(source):
        send_out(dir_ref.at[source], dir_out.at[source], dir_sem.at[source])

    moments = ((fq, sq), (fk, sk))
    for side, cols in enumerate(pieces):
        first, second = moments[side]
        dir_ref[me, :, cols] = moment_update(scaled[:, cols], first[...], second[...])[2]
        for i in range(1, outer):
            start(dir_copy(me, i - 1, level(i) * PAIR + x, side))
        start(dir_copy(me, outer - 1, mate, side))
    send_out(scaled_ref, scaled_out, out_sem.at[1])
    dir_store(me)
    for i in range(outer):
        source = level(i) * PAIR + (1 - x)
        master_copy(source, 0, mate).wait_recv()
    send_out(master_ref, master_out, out_sem.at[2])
    for side in range(len(pieces)):
        for i in range(1, outer):
            source = level(outer - i) * PAIR + x
            copy = dir_copy(source, outer - 1 + i, mate, side)
            copy.wait_recv()
            start(copy)
            if side == len(pieces) - 1:
                dir_store(source)
    for i in range(outer):
        source = level(outer - i) * PAIR + (1 - x)
        for side in range(len(pieces)):
            dir_copy(source, 0, mate, side).wait_recv()
        dir_store(source)
    for copy, when in pending:
        if when is None:
            copy.wait_send()
        else:
            pl.when(when)(copy.wait_send)
    for copy in stores:
        copy.wait()


def apply_kernel(
    scaled_ref,
    dir_ref,
    master_ref,
    basis_ref,
    bq,
    bk,
    fq,
    sq,
    fk,
    sk,
    uq_first_new,
    uq_second_new,
    uq_step,
    uq_copy,
    uk_first_new,
    uk_second_new,
    uk_step,
    uk_copy,
):
    n, rows, width = dir_ref.shape
    deep = basis_ref.shape[2]
    rank = n * rows
    width_q = fq.shape[1]
    for which, cols, own, first, second, first_new, second_new, step, fresh in (
        (0, slice(0, width_q), bq, fq, sq, uq_first_new, uq_second_new, uq_step, uq_copy),
        (1, slice(width_q, width), bk, fk, sk, uk_first_new, uk_second_new, uk_step, uk_copy),
    ):
        span = cols.stop - cols.start
        moved = moment_update(scaled_ref[:, cols], first[...], second[...])
        first_new[...] = moved[0]
        second_new[...] = moved[1]
        heading = dir_ref[:, :, cols].reshape(rank, span)
        step[...] = jnp.dot(own[...], heading, preferred_element_type=F32)
        factor = basis_ref[:, which].reshape(n * deep, rank)
        whole = jnp.dot(factor, heading, preferred_element_type=F32)
        master = master_ref[:, :, cols].reshape(n * deep, span).astype(F32)
        fresh[...] = (master - step_size * whole).astype(BF16)


def kernel_body(
    n,
    tp_size,
    q_latent,
    q_grad,
    uq_master,
    uq_basis,
    uq_first,
    uq_second,
    kv_latent,
    k_grad,
    uk_master,
    uk_basis,
    uk_first,
    uk_second,
):
    outer = n // PAIR
    tokens, latent = q_latent.shape
    deep, rank = uq_basis.shape
    rows = rank // n
    width_q, width_k = q_grad.shape[1], k_grad.shape[1]
    width = width_q + width_k
    dma = pltpu.SemaphoreType.DMA
    vmem = pl.BlockSpec(memory_space=pltpu.VMEM)
    args = (
        q_latent, q_grad, kv_latent, k_grad, uq_basis, uk_basis,
        uq_master, uk_master, uq_first, uq_second, uk_first, uk_second,
    )
    scaled, heading, master, basis = pl.pallas_call(
        functools.partial(exchange_kernel, n, tp_size),
        out_shape=(
            jax.ShapeDtypeStruct((rows, width), F32),
            jax.ShapeDtypeStruct((n, rows, width), BF16),
            jax.ShapeDtypeStruct((n, deep, width), BF16),
            jax.ShapeDtypeStruct((n, 2, deep, rank), BF16),
        ),
        in_specs=[pl.BlockSpec(memory_space=pl.ANY)] * len(args),
        out_specs=(pl.BlockSpec(memory_space=pl.ANY),) * 4,
        scratch_shapes=[
            pltpu.VMEM((rows, width), F32),
            pltpu.VMEM((n, rows, width), BF16),
            pltpu.VMEM((n, deep, width), BF16),
            pltpu.VMEM((n, 2, deep, rank), BF16),
            pltpu.VMEM(q_latent.shape, BF16),
            pltpu.VMEM(q_grad.shape, BF16),
            pltpu.VMEM(kv_latent.shape, BF16),
            pltpu.VMEM(k_grad.shape, BF16),
            pltpu.VMEM(uq_master.shape, F32),
            pltpu.VMEM(uk_master.shape, F32),
            pltpu.VMEM(uq_first.shape, F32),
            pltpu.VMEM(uq_second.shape, F32),
            pltpu.VMEM(uk_first.shape, F32),
            pltpu.VMEM(uk_second.shape, F32),
            pltpu.VMEM((latent, width_q), F32),
            pltpu.VMEM((latent, width_k), F32),
            pltpu.VMEM((n, rows, width), F32),
            pltpu.VMEM((outer, rows, width), BF16),
            pltpu.VMEM((outer, rows, width), BF16),
            pltpu.VMEM((outer, rows, width), BF16),
            pltpu.VMEM((outer, rows, width), BF16),
            pltpu.VMEM((8, 128), F32),
            pltpu.VMEM((tp_size, 8, 128), F32),
            pltpu.VMEM((8, 128), F32),
            pltpu.VMEM((n, 8, 128), F32),
            dma((len(args),)),
            dma((3,)),
            dma((n,)),
            dma((2 * outer - 1,)),
            dma((n,)),
            dma((n,)),
            dma((n,)),
            dma((4 * outer - 3,)),
            dma((n,)),
            dma((2 * outer - 1, 2)),
            dma((n, 2)),
            dma((outer, 2)),
            dma((outer, 2)),
            dma((outer, 2)),
            dma((outer, 2)),
            dma((tp_size,)),
            dma((tp_size,)),
            dma((n,)),
            dma((n,)),
        ],
        compiler_params=pltpu.CompilerParams(
            collective_id=0, has_side_effects=True, vmem_limit_bytes=VMEM_BYTES
        ),
        name="exchange",
    )(*args)
    shapes = tuple(
        jax.ShapeDtypeStruct(shape, dtype)
        for span in (width_q, width_k)
        for shape, dtype in (
            ((rows, span), F32),
            ((rows, span), F32),
            ((deep, span), F32),
            ((latent, span), BF16),
        )
    )
    return tuple(
        pl.pallas_call(
            apply_kernel,
            out_shape=shapes,
            in_specs=[vmem] * 10,
            out_specs=(vmem,) * 8,
            name="apply",
        )(
            scaled, heading, master, basis, uq_basis, uk_basis,
            uq_first, uq_second, uk_first, uk_second,
        )
    )


def across_tokens(left, right):
    return lax.dot_general(
        left, right, (((0,), (0,)), ((), ())), preferred_element_type=jnp.float32
    )


def across_latent(left, right):
    return lax.dot_general(
        left,
        right,
        (((0,), (0,)), ((), ())),
        precision=lax.Precision.HIGHEST,
        preferred_element_type=jnp.float32,
    )


def moment_update(scaled, first_old, second_old):
    first_new = first_decay * first_old + (1.0 - first_decay) * scaled
    second_new = second_decay * second_old + (1.0 - second_decay) * scaled * scaled
    heading = (first_new / (jnp.sqrt(second_new) + root_guard)).astype(jnp.bfloat16)
    return (first_new, second_new, heading)


def body(
    q_latent,
    q_grad,
    uq_master,
    uq_basis,
    uq_first,
    uq_second,
    kv_latent,
    k_grad,
    uk_master,
    uk_basis,
    uk_first,
    uk_second,
):
    q_width = q_grad.shape[1]
    q_whole, k_whole = (
        lax.all_gather(uq_basis, "fs", axis=0, tiled=True),
        lax.all_gather(uk_basis, "fs", axis=0, tiled=True),
    )
    q_factor = q_whole.astype(jnp.float32)
    k_factor = k_whole.astype(jnp.float32)
    q_partial = across_tokens(q_latent, q_grad)
    k_partial = across_tokens(kv_latent, k_grad)
    projected = lax.psum_scatter(
        jnp.concatenate(
            [across_latent(q_factor, q_partial), across_latent(k_factor, k_partial)], axis=1
        ),
        "fs",
        scatter_dimension=0,
        tiled=True,
    )
    squares_sum = lax.psum(jnp.sum(projected * projected), ("fs", "tp"))
    entry_count = (
        projected.shape[0] * projected.shape[1] * lax.axis_size("fs") * lax.axis_size("tp")
    )
    root_mean = jnp.sqrt(squares_sum / entry_count + mean_guard)
    scaled = projected / root_mean
    uq_first_new, uq_second_new, q_heading = moment_update(scaled[:, :q_width], uq_first, uq_second)
    uk_first_new, uk_second_new, k_heading = moment_update(scaled[:, q_width:], uk_first, uk_second)
    q_dir, k_dir = (
        lax.all_gather(q_heading, "fs", axis=0, tiled=True),
        lax.all_gather(k_heading, "fs", axis=0, tiled=True),
    )
    uq_step = jnp.dot(uq_basis, q_dir, preferred_element_type=jnp.float32)
    uk_step = jnp.dot(uk_basis, k_dir, preferred_element_type=jnp.float32)
    q_fresh = (uq_master - step_size * uq_step).astype(jnp.bfloat16)
    k_fresh = (uk_master - step_size * uk_step).astype(jnp.bfloat16)
    uq_copy, uk_copy = (
        lax.all_gather(q_fresh, "fs", axis=0, tiled=True),
        lax.all_gather(k_fresh, "fs", axis=0, tiled=True),
    )
    return (
        uq_first_new,
        uq_second_new,
        uq_step,
        uq_copy,
        uk_first_new,
        uk_second_new,
        uk_step,
        uk_copy,
    )


def chosen_body(n, tp_size, *args):
    deep, rank = args[3].shape
    tiled = n > 2 * PAIR and n % PAIR == 0 and tp_size % PAIR == 0 and rank % (16 * n) == 0 and deep % 16 == 0
    lanes = args[1].shape[1] % 128 == 0 and args[7].shape[1] % 128 == 0 and rank % 128 == 0
    if tiled and lanes:
        return kernel_body(n, tp_size, *args)
    return body(*args)


def solution(mesh):
    return jax.shard_map(
        functools.partial(chosen_body, mesh.shape["fs"], mesh.shape["tp"]),
        mesh=mesh,
        in_specs=(
            P("fs", None),
            P("fs", "tp"),
            P("fs", "tp"),
            P("fs", None),
            P("fs", "tp"),
            P("fs", "tp"),
            P("fs", None),
            P("fs", "tp"),
            P("fs", "tp"),
            P("fs", None),
            P("fs", "tp"),
            P("fs", "tp"),
        ),
        out_specs=(
            P("fs", "tp"),
            P("fs", "tp"),
            P("fs", "tp"),
            P(None, "tp"),
            P("fs", "tp"),
            P("fs", "tp"),
            P("fs", "tp"),
            P(None, "tp"),
        ),
        check_vma=False,
    )
```
